32 devices in a mesh: grp: 2 (over y), ep: 8 (over z, core), tp: 2 (over x).
Axes of the slice: x: 2, y: 2, z: 4, core: 2. Of those that a mesh axis runs over, the one named last changes fastest.
Arguments:
- tokens: bfloat16 [3072, 2048], P(('grp', 'ep')), parts along dimension 0, may hold values from -6 to 6
- norm_gain: float32 [2048], replicated, may hold values from 0.1 to 1.9
- w_gate: bfloat16 [8, 2048, 1024], P('ep', None, 'tp'), may hold values from -0.3125 to 0.3125
- w_up: bfloat16 [8, 2048, 1024], P('ep', None, 'tp'), may hold values from -0.3125 to 0.3125
- w_down: bfloat16 [8, 1024, 2048], P('ep', 'tp'), may hold values from -0.09375 to 0.09375
- expert_ids: int32 [3072, 4], P(('grp', 'ep')), parts along dimension 0, may hold values from 0 to 7, all different within a row; in each aligned block of 192 rows (0 to 191, 192 to 383, ...) at most 128 rows name the same one
- gate_weights: float32 [3072, 4], P(('grp', 'ep')), parts along dimension 0, may hold values from 0.1 to 1
Outputs:
- mixed: bfloat16 [3072, 2048], P(('grp', 'ep'), 'tp'), parts along dimension 0
The draws below stay inside these ranges and needn't reach their ends.
There are 2 independent parts, one for each index of `grp`. The reference program is written for one: setup_inputs(seed, part) draws one part's arguments, and reference() takes and returns one part's arrays. A program takes and returns all parts, laid end to end along the dimension named above; an argument that names none is the same for every part. Nothing has to cross between parts.
Inputs may be any that keep to these rules, and one draw needn't show every extreme that they name: `expert_ids`: each row names 4 different experts; among the rows of one index of ep, no expert is named by more than 128 rows, a bound that some block reaches.
All inputs are finite; a program needn't handle non-finite values.
Results may differ from the reference program's by a relative error of at most 0.012.
Values may be sent and summed in bfloat16 or wider, within the bound.
No kernel may reach another device: no remote copies, remote signals or barrier semaphores. Data moves between devices by JAX's collectives and lax.ppermute only.
A program may use at most 64 MiB of HBM per device.

```python
import math
import jax
import jax.numpy as jnp
import numpy as np
from jax import lax

D = 2048
FF = 1024
TOP_K = 4
TOK_DEV = 192
EXPERTS = 8
CAP = 128
TOKENS = 1536
N_EP = 8
N_TP = 2


def shard_levels(own_key, shape, cuts, least, largest):
    def one(dim, parts):
        steps = jax.random.uniform(jax.random.fold_in(jax.random.fold_in(own_key, 6), dim), (parts,), jnp.float32, least / len(cuts), largest / len(cuts))
        return jnp.repeat(jnp.exp(steps), shape[dim] // parts).reshape((-1,) + (1,) * (len(shape) - dim - 1))

    factor_of = one(*cuts[0])
    for cut in cuts[1:]:
        factor_of = factor_of * one(*cut)
    return factor_of


def deal_out(own_key, own, number, rows, count, top, most, skew):
    order = jax.random.permutation(own_key, count)
    heavy_load, ordinary = portions_of(count, rows * top, most, skew, True), portions_of(count, rows * top, most, skew, False)
    places = jnp.arange(count)

    def named(lengths, offset_by):
        used = int((lengths > 0).sum())
        fixed = max(1, used // 4)
        moved = fixed + (places - fixed + offset_by * (used - fixed)) % max(1, count - fixed)
        return jnp.zeros((count,), jnp.int32).at[order[jnp.where(places < fixed, places, moved)]].set(jnp.asarray(lengths, jnp.int32))

    lengths = jnp.where(number % 4 == 0, named(heavy_load, number // 4), named(ordinary, number - number // 4 - 1))
    mixed = jax.random.permutation(jax.random.fold_in(own, 3), count)
    donor, taker = mixed[0:count // 2 * 2:2], mixed[1:count // 2 * 2:2]
    room = jnp.minimum(lengths[donor] - 1, most - lengths[taker]) // 2
    room = jnp.where((donor == order[0]) | (taker == order[0]) | (lengths[taker] == 0), 0, jnp.maximum(room, 0))
    moved = jax.random.randint(jax.random.fold_in(own, 4), (count // 2,), 0, 1 << 20) % (room + 1)
    lengths = lengths.at[donor].add(-moved).at[taker].add(moved)
    items = jnp.searchsorted(jnp.cumsum(lengths), jnp.arange(rows * top), side="right").astype(jnp.int32)
    table = items.reshape(top, rows).T
    table = table[jax.random.permutation(jax.random.fold_in(own, 1), rows)]
    offset_by = jax.random.randint(jax.random.fold_in(own, 2), (rows, 1), 0, top)
    return jnp.take_along_axis(table, (jnp.arange(top)[None, :] + offset_by) % top, axis=1)


def portions_of(amount, total, bound, skew, full):
    portions = [(1 << 20) // math.isqrt(standing ** skew) + 1 for standing in range(1, amount + 1)]
    largest = bound if full else min(bound, max(-(-total // amount), total * portions[0] // sum(portions)))
    least = 1 if total - largest >= amount - 1 else 0
    holding, spare = [largest] + [least] * (amount - 1), total - largest - least * (amount - 1)
    while spare > 0:
        candidates = [i for i in range(1, amount) if holding[i] < largest] or [i for i in range(1, amount) if holding[i] < bound]
        whole, left = sum([portions[i] for i in candidates]), spare
        for i in candidates:
            addition = min(bound - holding[i], max(1, left * portions[i] // whole), spare)
            holding[i] = holding[i] + addition
            spare = spare - addition
    return np.array(holding)


def normal_values(key, shape, spread, limit, pieces=(), kind=jnp.bfloat16):
    drawn = spread * jax.random.normal(key, shape, jnp.float32)
    if pieces:
        drawn = drawn * shard_levels(key, shape, pieces, -0.22, 0.18)
    return jnp.clip(drawn, -limit, limit).astype(kind)


def setup_inputs(seed: int = 0, part: int = 0) -> dict:
    key_list = jax.random.split(jax.random.key(seed), 8)
    part_keys = jax.random.split(jax.random.fold_in(key_list[7], part), 8)
    tokens = normal_values(part_keys[0], (TOKENS, D), 1.0, 6.0, ((0, 8),))
    norm_gain = jnp.clip(1.0 + 0.18 * jax.random.normal(key_list[1], (D,), jnp.float32), 0.1, 1.9)
    w_gate = normal_values(key_list[2], (EXPERTS, D, FF), (D // 6) ** -0.5, 0.3125, ((0, 8), (2, 2)))
    w_up = normal_values(key_list[3], (EXPERTS, D, FF), (D // 6) ** -0.5, 0.3125, ((0, 8), (2, 2)))
    w_down = normal_values(key_list[4], (EXPERTS, FF, D), (FF * 4) ** -0.5, 0.09375, ((0, 8), (1, 2)))
    expert_ids_keys = jax.random.split(jax.random.fold_in(part_keys[5], 1), TOKENS // TOK_DEV)
    expert_ids_turns = jax.random.permutation(jax.random.fold_in(part_keys[5], 3), TOKENS // TOK_DEV)
    expert_ids = jax.vmap(lambda own, number: deal_out(jax.random.fold_in(part_keys[5], 2), own, number, TOK_DEV, EXPERTS, TOP_K, CAP, 1))(expert_ids_keys, expert_ids_turns).reshape((TOKENS, TOP_K))
    gate_weights = jnp.clip(0.1 + 0.9 * jax.random.uniform(part_keys[6], (TOKENS, TOP_K), jnp.float32) ** shard_levels(part_keys[6], (TOKENS, TOP_K), ((0, 8),), -0.2, 0.2), 0.1, 1.0)
    return {"tokens": tokens, "norm_gain": norm_gain, "w_gate": w_gate, "w_up": w_up, "w_down": w_down, "expert_ids": expert_ids, "gate_weights": gate_weights}


epsilon = 1e-06
clamp_limit = 7.0
swish_alpha = 1.702

def rms_norm(tokens, norm_gain):
    widened = tokens.astype(jnp.float32)
    scaled = widened * lax.rsqrt(lax.optimization_barrier(jnp.mean(widened * widened, axis=-1, keepdims=True)) + epsilon)
    return (scaled * norm_gain).astype(jnp.bfloat16)

def reference(tokens, norm_gain, w_gate, w_up, w_down, expert_ids, gate_weights):
    normed = rms_norm(tokens, norm_gain)
    src_ids = expert_ids.reshape(N_EP, TOK_DEV * TOP_K).astype(jnp.int32)
    onehot = (src_ids[:, :, None] == jnp.arange(EXPERTS, dtype=jnp.int32)[None, None, :]).astype(jnp.int32)
    before = jnp.cumsum(onehot, axis=1) - onehot
    slot_index = lax.optimization_barrier(jnp.sum(before * onehot, axis=2)).astype(jnp.int32)
    source = jnp.arange(N_EP, dtype=jnp.int32)[:, None]
    row_index = (src_ids * (N_EP * CAP) + source * CAP + slot_index).astype(jnp.int32)
    owner_tok = (source * TOK_DEV + jnp.arange(TOK_DEV * TOP_K, dtype=jnp.int32)[None, :] // TOP_K).astype(jnp.int32)
    slot_table = jnp.full((EXPERTS * N_EP * CAP,), TOKENS, jnp.int32)
    slot_table = slot_table.at[row_index.reshape(-1)].set(owner_tok.reshape(-1)).reshape(EXPERTS, N_EP * CAP)
    padded = jnp.concatenate([normed, jnp.zeros((1, D), jnp.bfloat16)], axis=0)

    def expert_fn(packed):
        slot_rows, gate_mat, up_mat, down_mat = packed
        expert_rows = padded[slot_rows]
        gate_pre = jnp.dot(expert_rows, gate_mat, preferred_element_type=jnp.float32)
        up_pre = jnp.dot(expert_rows, up_mat, preferred_element_type=jnp.float32)
        gated = jnp.minimum(gate_pre, clamp_limit)
        linear = jnp.clip(up_pre, -clamp_limit, clamp_limit)
        activated = (gated * jax.nn.sigmoid(swish_alpha * gated) * (linear + 1.0)).astype(jnp.bfloat16)
        act_blocks = activated.reshape(-1, N_TP, FF // N_TP).astype(jnp.float32)
        down_blocks = down_mat.reshape(N_TP, FF // N_TP, D).astype(jnp.float32)
        partial_value = jnp.einsum('rtf,tfd->rtd', act_blocks, down_blocks).astype(jnp.bfloat16)
        partial_value = lax.optimization_barrier(partial_value)
        return lax.optimization_barrier(jnp.sum(partial_value.astype(jnp.float32), axis=1)).astype(jnp.bfloat16)
    expert_out = lax.map(expert_fn, (slot_table, w_gate, w_up, w_down))
    picked = expert_out.reshape(EXPERTS * N_EP * CAP, D)[row_index.reshape(-1)]
    picked = picked.reshape(TOKENS, TOP_K, D).astype(jnp.float32)
    return lax.optimization_barrier(jnp.sum(picked * gate_weights[:, :, None], axis=1)).astype(jnp.bfloat16)
```

```python
import functools

import jax
import jax.numpy as jnp
from jax import lax
from jax.experimental import pallas as pl
from jax.experimental.pallas import tpu as pltpu
from jax.sharding import PartitionSpec as P

epsilon = 1e-06
clamp_limit = 7.0
swish_alpha = 1.702


def rms_norm(tokens, norm_gain):
    widened = tokens.astype(jnp.float32)
    scaled = widened * lax.rsqrt(jnp.mean(widened * widened, axis=-1, keepdims=True) + epsilon)
    return (scaled * norm_gain).astype(jnp.bfloat16)


def slot_body(tokens, norm_gain, w_gate, w_up, w_down, expert_ids, gate_weights):
    tok_rows, model_width = tokens.shape
    top_count = expert_ids.shape[1]
    ep_count = lax.axis_size("ep")
    local_experts = w_gate.shape[0]
    experts_all = local_experts * ep_count
    capacity = min(tok_rows, tok_rows * top_count * 4 // (3 * experts_all))
    normed = rms_norm(tokens, norm_gain)
    flat_ids = expert_ids.reshape(-1)
    onehot = (flat_ids[:, None] == jnp.arange(experts_all, dtype=jnp.int32)[None, :]).astype(
        jnp.int32
    )
    before = jnp.cumsum(onehot, axis=0) - onehot
    slot_index = jnp.sum(before * onehot, axis=1)
    dest_row = flat_ids * capacity + slot_index
    owner_tok = jnp.arange(tok_rows * top_count, dtype=jnp.int32) // top_count
    slot_table = (
        jnp.full((experts_all * capacity,), tok_rows, jnp.int32).at[dest_row].set(owner_tok)
    )
    padded = jnp.concatenate([normed, jnp.zeros((1, model_width), jnp.bfloat16)], axis=0)
    send_buffer = padded[slot_table].reshape(experts_all, capacity, model_width)
    received = lax.all_to_all(send_buffer, "ep", split_axis=0, concat_axis=0, tiled=True)
    expert_rows = received.reshape(ep_count, local_experts, capacity, model_width)
    gate_pre = jnp.einsum("sjcd,jdf->sjcf", expert_rows, w_gate, preferred_element_type=jnp.float32)
    up_pre = jnp.einsum("sjcd,jdf->sjcf", expert_rows, w_up, preferred_element_type=jnp.float32)
    gated = jnp.minimum(gate_pre, clamp_limit)
    linear = jnp.clip(up_pre, -clamp_limit, clamp_limit)
    activated = (gated * jax.nn.sigmoid(swish_alpha * gated) * (linear + 1.0)).astype(jnp.bfloat16)
    partial_value = jnp.einsum(
        "sjcf,jfd->sjcd", activated, w_down, preferred_element_type=jnp.float32
    ).astype(jnp.bfloat16)
    summed = (
        lax.psum_scatter(partial_value, "tp", scatter_dimension=3, tiled=True)
        .astype(jnp.float32)
        .astype(jnp.bfloat16)
    )
    returned = lax.all_to_all(summed, "ep", split_axis=0, concat_axis=0, tiled=True)
    returned = returned.reshape(experts_all * capacity, returned.shape[3])
    picked = returned[dest_row].reshape(tok_rows, top_count, returned.shape[1]).astype(jnp.float32)
    return jnp.sum(picked * gate_weights[:, :, None], axis=1).astype(jnp.bfloat16)


def expert_kernel(
    tile, where_ref, a_mine, a_other, b_mine, b_other, a_scale, b_scale, wg, wu, wd,
    keep, send, rows, act,
):
    tok_rows, half = a_mine.shape
    hidden = wg.shape[1]
    own, expert = where_ref[0], where_ref[1]
    mine = pl.ds(pl.multiple_of(own * half, half), half)
    other = pl.ds(pl.multiple_of((1 - own) * half, half), half)
    rows[:tok_rows, mine] = a_mine[...]
    rows[:tok_rows, other] = a_other[...]
    rows[tok_rows:, mine] = b_mine[...]
    rows[tok_rows:, other] = b_other[...]
    for j in range(hidden // tile):
        cols = pl.ds(j * tile, tile)
        gate_pre = jnp.dot(rows[...], wg[:, cols], preferred_element_type=jnp.float32)
        up_pre = jnp.dot(rows[...], wu[:, cols], preferred_element_type=jnp.float32)
        gated = jnp.minimum(gate_pre, clamp_limit)
        linear = jnp.clip(up_pre, -clamp_limit, clamp_limit)
        act[:, cols] = (gated * jax.nn.sigmoid(swish_alpha * gated) * (linear + 1.0)).astype(
            jnp.bfloat16
        )
    scale = jnp.concatenate([a_scale[...], b_scale[...]], axis=0)
    lane = lax.broadcasted_iota(jnp.int32, scale.shape, 1)
    scale = jnp.sum(jnp.where(lane == expert, scale, 0.0), axis=1, keepdims=True)
    for n in range(2 * half // tile):
        part, offset = divmod(n * tile, half)
        base = (1 - own) * half if part == 0 else own * half
        cols = pl.ds(pl.multiple_of(base + offset, tile), tile)
        product = jnp.dot(act[...], wd[:, cols], preferred_element_type=jnp.float32) * scale
        product = product.astype(jnp.bfloat16)
        keep[:, pl.ds(n * tile, tile)] = product[:tok_rows]
        send[:, pl.ds(n * tile, tile)] = product[tok_rows:]


def run_expert(where, pieces, scales, w_gate, w_up, w_down):
    tok_rows, half = pieces[0].shape
    width, hidden = w_gate.shape
    tile = 256 if hidden % 256 == 0 and half % 256 == 0 else 128
    out = jax.ShapeDtypeStruct((tok_rows, width), jnp.bfloat16)
    vmem = pl.BlockSpec(memory_space=pltpu.VMEM)
    flops = 2 * tok_rows * 2 * 3 * width * hidden
    return pl.pallas_call(
        functools.partial(expert_kernel, tile),
        out_shape=(out, out),
        in_specs=[pl.BlockSpec(memory_space=pltpu.SMEM)] + [vmem] * 9,
        out_specs=(vmem, vmem),
        scratch_shapes=[
            pltpu.VMEM((2 * tok_rows, width), jnp.bfloat16),
            pltpu.VMEM((2 * tok_rows, hidden), jnp.bfloat16),
        ],
        compiler_params=pltpu.CompilerParams(vmem_limit_bytes=32 * 1024 * 1024),
        cost_estimate=pl.CostEstimate(
            flops=flops, bytes_accessed=3 * width * hidden * 2, transcendentals=0
        ),
        name="expert",
    )(where, *pieces, *scales, w_gate, w_up, w_down)


def dense_body(tokens, norm_gain, w_gate, w_up, w_down, expert_ids, gate_weights):
    tok_rows, width = tokens.shape
    ep_count = lax.axis_size("ep")
    half = width // 2
    own = lax.axis_index("tp")
    place = lax.axis_index("ep")

    def swap(value, axis, bit):
        count = lax.axis_size(axis)
        return lax.ppermute(value, axis, [(i, i ^ bit) for i in range(count)])

    def add(*terms):
        return functools.reduce(jnp.add, [t.astype(jnp.float32) for t in terms]).astype(
            jnp.bfloat16
        )

    experts = jnp.arange(ep_count, dtype=jnp.int32)
    scale = jnp.sum(
        jnp.where(expert_ids[:, :, None] == experts, gate_weights[:, :, None], 0.0), axis=1
    )
    scales = lax.all_gather(scale, "ep")
    normed = rms_norm(tokens, norm_gain)
    mine = lax.dynamic_slice_in_dim(normed, own * half, half, 1)
    other = lax.dynamic_slice_in_dim(normed, (1 - own) * half, half, 1)
    bits = [1 << i for i in range(1, (ep_count - 1).bit_length())]

    blocks = {0: mine}
    for bit in reversed(bits):
        for mask in list(blocks):
            blocks[mask | bit] = swap(blocks[mask], "ep", bit)
    where = jnp.stack([own, place])
    sums = {}
    for mask in blocks:
        a_mine = blocks[mask]
        a_other = other if mask == 0 else swap(a_mine, "tp", 1)
        b_mine, b_other = swap(a_mine, "ep", 1), swap(a_other, "ep", 1)
        a_scale = lax.dynamic_index_in_dim(scales, place ^ mask, 0, False)
        b_scale = lax.dynamic_index_in_dim(scales, place ^ mask ^ 1, 0, False)
        keep, send = run_expert(
            where, (a_mine, a_other, b_mine, b_other), (a_scale, b_scale),
            w_gate[0], w_up[0], w_down[0],
        )
        came = swap(send, "ep", 1)
        crossed = swap(add(keep[:, :half], came[:, :half]), "tp", 1)
        sums[mask] = (keep[:, half:], came[:, half:], crossed)
    for bit in bits:
        for mask in [m for m in sums if m & bit]:
            moved = swap(add(*sums.pop(mask)), "ep", bit)
            sums[mask ^ bit] = (*sums[mask ^ bit], moved)
    return add(*sums[0])


def solution(mesh):
    placed = (
        P(("grp", "ep"), None),
        P(),
        P("ep", None, "tp"),
        P("ep", None, "tp"),
        P("ep", "tp", None),
        P(("grp", "ep"), None),
        P(("grp", "ep"), None),
    )

    def body(tokens, norm_gain, w_gate, w_up, w_down, expert_ids, gate_weights):
        ep_count, tp_count = mesh.shape["ep"], mesh.shape["tp"]
        experts_all = w_gate.shape[0] * ep_count
        slots = tokens.shape[0] * expert_ids.shape[1] * 4 // 3
        dense = (
            ep_count & (ep_count - 1) == 0
            and tp_count == 2
            and experts_all == ep_count
            and tokens.shape[0] * ep_count <= 2 * slots
        )
        step = dense_body if dense else slot_body
        return step(tokens, norm_gain, w_gate, w_up, w_down, expert_ids, gate_weights)

    return jax.shard_map(
        body, mesh=mesh, in_specs=placed, out_specs=P(("grp", "ep"), "tp"), check_vma=False
    )
```
